32 devices in a mesh: fs: 4 (over y, x), tp: 8 (over z, core).
Axes of the slice: x: 2, y: 2, z: 4, core: 2. Of those that a mesh axis runs over, the one named last changes fastest.
Arguments:
- saved_inputs: bfloat16 [2688, 4096], P('fs', 'tp'), may hold values from -6 to 6
- proj_cotangent: bfloat16 [2688, 4096], P('fs', 'tp'), may hold values from -0.115722656 to 0.115722656
- saved_hidden: bfloat16 [2688, 4096], P('fs', 'tp'), may hold values from -6 to 6
- out_cotangent: bfloat16 [2688, 4096], P('fs', 'tp'), may hold values from -0.115722656 to 0.115722656
- factors: bfloat16 [2, 4096, 128], replicated, may hold values from -0.46875 to 0.46875
- w_proj: float32 [4096, 4096], P('fs', 'tp'), may hold values from -0.09375 to 0.09375
- w_out: float32 [4096, 4096], P('tp', 'fs'), may hold values from -0.09375 to 0.09375
- moment_first: float32 [2, 128, 4096], P(None, None, 'tp'), may hold values from -1.8 to 1.8
- moment_second: float32 [2, 128, 4096], P(None, None, 'tp'), may hold values from 0.05 to 1
Outputs:
- proj_next: float32 [4096, 4096], P('fs', 'tp')
- out_next: float32 [4096, 4096], P('tp', 'fs')
- proj_copy: bfloat16 [4096, 4096], P(None, 'tp')
- out_copy: bfloat16 [4096, 4096], P('tp')
- first_next: float32 [2, 128, 4096], P(None, None, 'tp')
- second_next: float32 [2, 128, 4096], P(None, None, 'tp')
The draws below stay inside these ranges and needn't reach their ends.
All inputs are finite; a program needn't handle non-finite values.
Results may differ from the reference program's by a relative error of at most 0.001.
Values may be sent and summed in bfloat16 or wider, within the bound.
A program may use at most 64 MiB of HBM per device.

```python
import math
import jax
import jax.numpy as jnp
from jax import lax

D = 4096
E = 4096
RANK = 128
TOKENS = 2688


def draw_factors(key, part):
    base_key, rough_key = jax.random.split(jax.random.fold_in(key, 11))
    position = jnp.arange(D, dtype=jnp.float32) / max(D - 1, 1)
    rough = jnp.exp(jax.random.uniform(rough_key, (2, D, 1), jnp.float32, 0.0, math.log(4.0)))
    base = jnp.clip(jax.random.normal(base_key, (2, D, RANK), jnp.float32), -4.0, 4.0)
    rising = jnp.exp(position * math.log(3.0))
    values = base * rough * rising[None, :, None] * (0.5 / math.sqrt(D))
    return values.astype(jnp.bfloat16)


def block_levels(key, dims, pieces, smallest, high):
    def one(axis_at, parts):
        draws = jax.random.uniform(jax.random.fold_in(jax.random.fold_in(key, 6), axis_at), (parts,), jnp.float32, smallest / len(pieces), high / len(pieces))
        return jnp.repeat(jnp.exp(draws), dims[axis_at] // parts).reshape((-1,) + (1,) * (len(dims) - axis_at - 1))

    factor_of = one(*pieces[0])
    for cut in pieces[1:]:
        factor_of = factor_of * one(*cut)
    return factor_of


def scatter_about(stream_key, dims, width, limit, pieces=(), kind=jnp.bfloat16):
    factor_of = block_levels(stream_key, dims, pieces, -0.22, 0.18) if pieces else 1.0
    entries = jax.random.normal(stream_key, dims, jnp.float32) * width * factor_of
    return jnp.minimum(jnp.maximum(entries, -limit), limit).astype(kind)


def setup_inputs(seed: int = 0) -> dict:
    keys = jax.random.split(jax.random.key(seed), 10)
    saved_inputs = scatter_about(keys[0], (TOKENS, D), 1.0, 6.0, ((0, 4), (1, 8)))
    proj_cotangent = scatter_about(keys[1], (TOKENS, E), (TOKENS ** -0.5), 0.115722656, ((0, 4), (1, 8)))
    saved_hidden = scatter_about(keys[2], (TOKENS, E), 1.0, 6.0, ((0, 4), (1, 8)))
    out_cotangent = scatter_about(keys[3], (TOKENS, D), (TOKENS ** -0.5), 0.115722656, ((0, 4), (1, 8)))
    factors = draw_factors(jax.random.fold_in(keys[9], 71), 0)
    w_proj = scatter_about(keys[5], (D, E), D ** -0.5, 0.09375, ((0, 4), (1, 8)), jnp.float32)
    w_out = scatter_about(keys[6], (E, D), E ** -0.5, 0.09375, ((0, 8), (1, 4)), jnp.float32)
    moment_first = scatter_about(keys[7], (2, RANK, E), 0.3, 1.8, ((2, 8),), jnp.float32)
    moment_second = jnp.clip(jnp.exp(math.log(1.0) - 2.9957323 * jax.random.uniform(keys[8], (2, RANK, E), jnp.float32) ** block_levels(keys[8], (2, RANK, E), ((2, 8),), -0.2, 0.2)), 0.05, 1.0)
    return {"saved_inputs": saved_inputs, "proj_cotangent": proj_cotangent, "saved_hidden": saved_hidden, "out_cotangent": out_cotangent, "factors": factors, "w_proj": w_proj, "w_out": w_out, "moment_first": moment_first, "moment_second": moment_second}


beta_first = 0.9
beta_second = 0.95
learn_rate = 0.02
epsilon = 1e-06

def reference(saved_inputs, proj_cotangent, saved_hidden, out_cotangent, factors, w_proj, w_out, moment_first, moment_second):
    highest = lax.Precision.HIGHEST
    factor_full = factors.astype(jnp.float32)
    grad_proj = jnp.dot(saved_inputs.T, proj_cotangent, preferred_element_type=jnp.float32)
    grad_out_t = jnp.dot(out_cotangent.T, saved_hidden, preferred_element_type=jnp.float32)
    small_grads = jnp.stack([jnp.dot(factor_full[0].T, grad_proj, precision=highest), jnp.dot(factor_full[1].T, grad_out_t, precision=highest)])
    first_next = beta_first * moment_first + (1.0 - beta_first) * small_grads
    second_next = beta_second * moment_second + (1.0 - beta_second) * small_grads * small_grads
    direction = first_next / (jnp.sqrt(second_next) + epsilon)
    update_full = jnp.einsum('kdr,kre->kde', factor_full, direction, precision=highest)
    norm_scale = lax.rsqrt(lax.optimization_barrier(jnp.mean(update_full * update_full, axis=(1, 2))) + epsilon)
    stepped = update_full * norm_scale[:, None, None]
    proj_next = w_proj - learn_rate * stepped[0]
    out_next = w_out - learn_rate * stepped[1].T
    return (proj_next, out_next, proj_next.astype(jnp.bfloat16), out_next.astype(jnp.bfloat16), first_next, second_next)
```

```python
import functools

import jax
import jax.numpy as jnp
from jax import lax
from jax.experimental import pallas as pl
from jax.experimental.pallas import tpu as pltpu
from jax.sharding import PartitionSpec as P

beta_first = 0.9
beta_second = 0.95
learn_rate = 0.02
epsilon = 1e-06
weight_gain = 2500.0
sub_steps = 2
MESH = pl.DeviceIdType.MESH


def encode(w):
    t = w * weight_gain
    t = t * t
    t = t * t
    t = t * t
    t = t * t
    return jnp.where(w < 0, -t, t).astype(jnp.bfloat16)


def decode(code):
    v = code.astype(jnp.float32)
    size = jnp.exp2(jnp.log2(jnp.abs(v)) * (1.0 / 16.0)) * (1.0 / weight_gain)
    return jnp.where(v < 0, -size, size)


def two_parts(x, axis):
    high = x.astype(jnp.bfloat16)
    low = (x - high.astype(jnp.float32)).astype(jnp.bfloat16)
    return jnp.concatenate([high, low], axis=axis)


def exchange_kernel(
    tp_count,
    entries,
    si_ref,
    pc_ref,
    sh_ref,
    oc_ref,
    f_ref,
    wp_ref,
    wo_ref,
    mf_ref,
    ms_ref,
    first_ref,
    second_ref,
    d0_ref,
    d1_ref,
    gp_ref,
    go_ref,
    cp,
    co,
    rows,
    rows_in,
    rows_all,
    part,
    part_in,
    grads,
    sq,
    sq_in,
    bulk_s,
    bulk_r,
    zs_s,
    zs_r,
    zg_s,
    zg_r,
    fs_s,
    fs_r,
    fg_s,
    fg_r,
    n_s,
    n_r,
):
    fs = lax.axis_index("fs")
    tp = lax.axis_index("tp")
    across_x = fs + 1 - 2 * lax.rem(fs, 2)
    across_y = lax.rem(fs + 2, 4)
    fs_peers = (across_x, across_y, 3 - fs)
    tp_peers = [lax.rem(tp + o, tp_count) for o in range(1, tp_count)]

    def send(src, dst, s_sem, r_sem, where):
        copy = pltpu.make_async_remote_copy(
            src_ref=src, dst_ref=dst, send_sem=s_sem, recv_sem=r_sem, device_id=where, device_id_type=MESH
        )
        copy.start()
        return copy

    barrier = pltpu.get_barrier_semaphore()
    for p in fs_peers:
        pl.semaphore_signal(barrier, inc=1, device_id={"fs": p}, device_id_type=MESH)
    for p in tp_peers:
        pl.semaphore_signal(barrier, inc=1, device_id={"tp": p}, device_id_type=MESH)
    cp[...] = encode(wp_ref[...])
    co[...] = encode(wo_ref[...])
    pl.semaphore_wait(barrier, 3 + len(tp_peers))
    bulk = [
        send(cp, gp_ref.at[0], bulk_s.at[0], bulk_r.at[0], {"fs": across_x}),
        send(co, go_ref.at[1], bulk_s.at[1], bulk_r.at[1], {"fs": across_y}),
        send(co, go_ref.at[0], bulk_s.at[2], bulk_r.at[2], {"fs": across_x}),
        send(cp, gp_ref.at[1], bulk_s.at[3], bulk_r.at[3], {"fs": across_y}),
    ]

    tokens, feats = si_ref.shape
    own = pl.ds(pl.multiple_of(tp * feats, feats), feats)
    rows[:tokens, :] = jnp.dot(si_ref[...], f_ref[0, own, :], preferred_element_type=jnp.float32)
    rows[tokens:, :] = jnp.dot(oc_ref[...], f_ref[1, own, :], preferred_element_type=jnp.float32)
    piece = rows_in.shape[1]

    def rows_of(i):
        return pl.ds(pl.multiple_of(i * piece, 8), piece)

    copies = [
        send(rows.at[rows_of(p), :], rows_in.at[i], zs_s.at[i], zs_r.at[i], {"tp": p})
        for i, p in enumerate(tp_peers)
    ]
    for c in copies:
        c.wait_recv()
    total = rows[rows_of(tp), :]
    for i in range(tp_count - 1):
        total = total + rows_in[i]
    rows_all[rows_of(tp), :] = total
    gathers = [
        send(rows_all.at[rows_of(tp), :], rows_all.at[rows_of(tp), :], zg_s.at[i], zg_r.at[i], {"tp": p})
        for i, p in enumerate(tp_peers)
    ]
    for c in copies:
        c.wait_send()
    for c in gathers:
        c.wait_recv()

    rank = f_ref.shape[2]
    for k, right in enumerate((pc_ref, sh_ref)):
        left = two_parts(rows_all[k * tokens : (k + 1) * tokens, :], 1)
        both = lax.dot_general(
            left, right[...], (((0,), (0,)), ((), ())), preferred_element_type=jnp.float32
        )
        part[k * rank : (k + 1) * rank, :] = both[:rank] + both[rank:]
    for c in gathers:
        c.wait_send()
    slab = part_in.shape[1]

    def slab_of(i):
        return pl.ds(pl.multiple_of(i * slab, 8), slab)

    copies = [
        send(part.at[slab_of(p), :], part_in.at[i], fs_s.at[i], fs_r.at[i], {"fs": p})
        for i, p in enumerate(fs_peers)
    ]
    for c in copies:
        c.wait_recv()
    grads[slab_of(fs), :] = (part[slab_of(fs), :] + part_in[0]) + (part_in[1] + part_in[2])
    gathers = [
        send(grads.at[slab_of(fs), :], grads.at[slab_of(fs), :], fg_s.at[i], fg_r.at[i], {"fs": p})
        for i, p in enumerate(fs_peers)
    ]
    bulk[0].wait_recv()
    bulk.append(send(gp_ref.at[0], gp_ref.at[2], bulk_s.at[4], bulk_r.at[4], {"fs": across_y}))
    bulk[1].wait_recv()
    bulk.append(send(go_ref.at[1], go_ref.at[2], bulk_s.at[5], bulk_r.at[5], {"fs": across_x}))
    for c in copies:
        c.wait_send()
    for c in gathers:
        c.wait_recv()
    small = grads[...]
    first = beta_first * mf_ref[...] + (1.0 - beta_first) * small
    second = beta_second * ms_ref[...] + (1.0 - beta_second) * small * small
    first_ref[...] = first
    second_ref[...] = second
    direction = first / (jnp.sqrt(second) + epsilon)
    for c in gathers:
        c.wait_send()

    d_model = f_ref.shape[1]
    step = d_model // 8
    squares = []
    for k in range(2):
        thin = two_parts(direction[k * rank : (k + 1) * rank], 0)

        def add(i, acc, k=k, thin=thin):
            f = f_ref[k, pl.ds(pl.multiple_of(i * step, step), step), :]
            u = jnp.dot(jnp.concatenate([f, f], axis=1), thin, preferred_element_type=jnp.float32)
            return acc + jnp.sum(u * u, axis=0, keepdims=True)

        acc = lax.fori_loop(0, 8, add, jnp.zeros((1, direction.shape[1]), jnp.float32))
        squares.append(jnp.sum(acc, axis=1, keepdims=True))
    row = lax.broadcasted_iota(jnp.int32, sq.shape, 0)
    sq[...] = jnp.where(row == 0, squares[0], squares[1])
    norms = [send(sq, sq_in.at[i], n_s.at[i], n_r.at[i], {"tp": p}) for i, p in enumerate(tp_peers)]
    for c in norms:
        c.wait_recv()
    total = sq[...]
    for i in range(tp_count - 1):
        total = total + sq_in[i]
    scale = -learn_rate * lax.rsqrt(total / entries + epsilon)
    d0_ref[...] = two_parts(direction[:rank] * scale[0:1, 0:1], 0)
    d1_ref[...] = two_parts(jnp.transpose(direction[rank:] * scale[1:2, 0:1]), 1)
    for c in norms:
        c.wait_send()
    for c in bulk[2:]:
        c.wait_recv()
    for c in bulk:
        c.wait_send()


def finish_kernel(
    me_ref, f0, f1, d0, d1, wp, wo, gp, go, mf, ms, pn, on, pcopy, ocopy, first, second
):
    i = pl.program_id(0)
    left = jnp.concatenate([f0[0], f0[0]], axis=1)
    right = jnp.concatenate([f1[0], f1[0]], axis=1)
    u0 = jnp.dot(left, d0[...], preferred_element_type=jnp.float32)
    u1 = lax.dot_general(d1[...], right, (((1,), (1,)), ((), ())), preferred_element_type=jnp.float32)

    @pl.when(i == 0)
    def _():
        first[...] = mf[...]
        second[...] = ms[...]

    @pl.when(i < sub_steps)
    def _():
        new = wp[...] + u0
        pn[...] = new
        pcopy[...] = new.astype(jnp.bfloat16)
        new = wo[...] + u1
        on[...] = new
        ocopy[...] = new.astype(jnp.bfloat16)

    @pl.when(i >= sub_steps)
    def _():
        pcopy[...] = (decode(gp[0]) + u0).astype(jnp.bfloat16)
        ocopy[...] = (decode(go[0]) + u1).astype(jnp.bfloat16)


def fast_body(si, pc, sh, oc, factors, w_proj, w_out, m1, m2):
    fs_count, tp_count = lax.axis_size("fs"), lax.axis_size("tp")
    kinds, d_model, rank = factors.shape
    tokens = si.shape[0]
    width = pc.shape[1]
    d_rows = w_proj.shape[0]
    f32, bf16 = jnp.float32, jnp.bfloat16
    mf, ms = m1.reshape(2 * rank, width), m2.reshape(2 * rank, width)
    vm = pl.BlockSpec(memory_space=pltpu.VMEM)
    anywhere = pl.BlockSpec(memory_space=pl.ANY)
    dma = lambda n: pltpu.SemaphoreType.DMA((n,))
    peers = tp_count - 1
    piece = 2 * tokens // tp_count
    slab = 2 * rank // fs_count
    first, second, d0, d1, gp, go = pl.pallas_call(
        functools.partial(exchange_kernel, tp_count, float(d_model * width * tp_count)),
        out_shape=(
            jax.ShapeDtypeStruct((2 * rank, width), f32),
            jax.ShapeDtypeStruct((2 * rank, width), f32),
            jax.ShapeDtypeStruct((2 * rank, width), bf16),
            jax.ShapeDtypeStruct((width, 2 * rank), bf16),
            jax.ShapeDtypeStruct((3, d_rows, width), bf16),
            jax.ShapeDtypeStruct((3, width, d_rows), bf16),
        ),
        in_specs=[vm] * 9,
        out_specs=(vm, vm, vm, vm, anywhere, anywhere),
        scratch_shapes=[
            pltpu.VMEM((d_rows, width), bf16),
            pltpu.VMEM((width, d_rows), bf16),
            pltpu.VMEM((2 * tokens, rank), f32),
            pltpu.VMEM((peers, piece, rank), f32),
            pltpu.VMEM((2 * tokens, rank), f32),
            pltpu.VMEM((2 * rank, width), f32),
            pltpu.VMEM((3, slab, width), f32),
            pltpu.VMEM((2 * rank, width), f32),
            pltpu.VMEM((8, 128), f32),
            pltpu.VMEM((peers, 8, 128), f32),
            dma(6),
            dma(6),
            dma(peers),
            dma(peers),
            dma(peers),
            dma(peers),
            dma(3),
            dma(3),
            dma(3),
            dma(3),
            dma(peers),
            dma(peers),
        ],
        compiler_params=pltpu.CompilerParams(
            collective_id=0, has_side_effects=True, vmem_limit_bytes=40 * 1024 * 1024
        ),
        name="exchange",
    )(si, pc, sh, oc, factors, w_proj, w_out, mf, ms)

    me = lax.axis_index("fs").astype(jnp.int32).reshape(1)
    n = sub_steps
    rows = d_rows // n

    def where(i, me):
        return (me[0] ^ (i // n)) * n + i % n

    def mine(i):
        return jnp.minimum(i, n - 1)

    def theirs(i):
        j = jnp.maximum(i - n, 0)
        return j // n, j % n

    whole = pl.BlockSpec((2 * rank, width), lambda i, me: (0, 0))
    pn, on, pcopy, ocopy, first, second = pl.pallas_call(
        finish_kernel,
        grid_spec=pltpu.PrefetchScalarGridSpec(
            num_scalar_prefetch=1,
            grid=(fs_count * n,),
            in_specs=[
                pl.BlockSpec((1, rows, rank), lambda i, me: (0, where(i, me), 0)),
                pl.BlockSpec((1, rows, rank), lambda i, me: (1, where(i, me), 0)),
                whole,
                pl.BlockSpec((width, 2 * rank), lambda i, me: (0, 0)),
                pl.BlockSpec((rows, width), lambda i, me: (mine(i), 0)),
                pl.BlockSpec((width, rows), lambda i, me: (0, mine(i))),
                pl.BlockSpec((1, rows, width), lambda i, me: (theirs(i)[0], theirs(i)[1], 0)),
                pl.BlockSpec((1, width, rows), lambda i, me: (theirs(i)[0], 0, theirs(i)[1])),
                whole,
                whole,
            ],
            out_specs=[
                pl.BlockSpec((rows, width), lambda i, me: (mine(i), 0)),
                pl.BlockSpec((width, rows), lambda i, me: (0, mine(i))),
                pl.BlockSpec((rows, width), lambda i, me: (where(i, me), 0)),
                pl.BlockSpec((width, rows), lambda i, me: (0, where(i, me))),
                whole,
                whole,
            ],
        ),
        out_shape=(
            jax.ShapeDtypeStruct(w_proj.shape, f32),
            jax.ShapeDtypeStruct(w_out.shape, f32),
            jax.ShapeDtypeStruct((d_model, width), bf16),
            jax.ShapeDtypeStruct((width, d_model), bf16),
            jax.ShapeDtypeStruct((2 * rank, width), f32),
            jax.ShapeDtypeStruct((2 * rank, width), f32),
        ),
        compiler_params=pltpu.CompilerParams(vmem_limit_bytes=40 * 1024 * 1024),
        name="finish",
    )(me, factors, factors, d0, d1, w_proj, w_out, gp, go, first, second)
    return pn, on, pcopy, ocopy, first.reshape(m1.shape), second.reshape(m2.shape)


def over_tokens(left_rows, right_rows, precise):
    return lax.dot_general(
        left_rows,
        right_rows,
        (((0,), (0,)), ((), ())),
        preferred_element_type=jnp.float32,
        precision=precise,
    )


def body(
    saved_inputs,
    proj_cotangent,
    saved_hidden,
    out_cotangent,
    factors,
    w_proj,
    w_out,
    moment_first,
    moment_second,
):
    highest = lax.Precision.HIGHEST
    fs_count = lax.axis_size("fs")
    tp_count = lax.axis_size("tp")
    d_model = factors.shape[1]
    hidden_width = proj_cotangent.shape[1]
    fs_rows = d_model // fs_count
    tp_feats = saved_inputs.shape[1]
    own_rows = lax.dynamic_slice_in_dim(factors, lax.axis_index("fs") * fs_rows, fs_rows, 1).astype(
        jnp.float32
    )
    own_feats = lax.dynamic_slice_in_dim(factors, lax.axis_index("tp") * tp_feats, tp_feats, 1)
    proj_rows = jnp.dot(saved_inputs, own_feats[0], preferred_element_type=jnp.float32)
    out_rows = jnp.dot(out_cotangent, own_feats[1], preferred_element_type=jnp.float32)
    proj_rows, out_rows = lax.psum((proj_rows, out_rows), "tp")
    partial_sums = jnp.stack(
        [
            over_tokens(proj_rows, proj_cotangent.astype(jnp.float32), highest),
            over_tokens(out_rows, saved_hidden.astype(jnp.float32), highest),
        ]
    )
    small_grads = lax.psum(partial_sums, "fs")
    first_next = beta_first * moment_first + (1.0 - beta_first) * small_grads
    second_next = beta_second * moment_second + (1.0 - beta_second) * small_grads * small_grads
    direction = first_next / (jnp.sqrt(second_next) + epsilon)
    update_full = jnp.einsum("kdr,kre->kde", own_rows, direction, precision=highest)
    squares = lax.psum(jnp.sum(update_full * update_full, axis=(1, 2)), ("fs", "tp"))
    norm_scale = lax.rsqrt(squares / (d_model * hidden_width * tp_count) + epsilon)
    stepped = update_full * norm_scale[:, None, None]
    proj_next = w_proj - learn_rate * stepped[0]
    out_next = w_out - learn_rate * stepped[1].T
    proj_copy, out_copy = (
        lax.all_gather(proj_next.astype(jnp.bfloat16), "fs", axis=0, tiled=True),
        lax.all_gather(out_next.astype(jnp.bfloat16), "fs", axis=1, tiled=True),
    )
    return (proj_next, out_next, proj_copy, out_copy, first_next, second_next)


def solution(mesh):
    placed = (
        P("fs", "tp"),
        P("fs", "tp"),
        P("fs", "tp"),
        P("fs", "tp"),
        P(),
        P("fs", "tp"),
        P("tp", "fs"),
        P(None, None, "tp"),
        P(None, None, "tp"),
    )
    planned = fast_body if mesh.shape["fs"] == 4 and mesh.shape["tp"] == 8 else body
    return jax.shard_map(
        planned,
        mesh=mesh,
        in_specs=placed,
        out_specs=(
            P("fs", "tp"),
            P("tp", "fs"),
            P(None, "tp"),
            P("tp", None),
            P(None, None, "tp"),
            P(None, None, "tp"),
        ),
        check_vma=False,
    )
```

```python
import functools

import jax
import jax.numpy as jnp
from jax import lax
from jax.experimental import pallas as pl
from jax.experimental.pallas import tpu as pltpu
from jax.sharding import PartitionSpec as P

beta_first = 0.9
beta_second = 0.95
learn_rate = 0.02
epsilon = 1e-06
weight_gain = 2500.0
code_top = 200.0
chunks = 4
MIB = 1024 * 1024
MESH = pl.DeviceIdType.MESH


def encode(x, gain, doublings):
    t = x * gain
    for _ in range(doublings):
        t = t * t
    return jnp.where(x < 0, -t, t).astype(jnp.bfloat16)


def decode(code, gain, doublings):
    v = code.astype(jnp.float32)
    size = jnp.exp2(jnp.log2(jnp.abs(v)) * (0.5**doublings)) * (1.0 / gain)
    return jnp.where(v < 0, -size, size)


def largest(x):
    top = jnp.max(jnp.max(jnp.abs(x), axis=0, keepdims=True), axis=1, keepdims=True)
    return jnp.maximum(top, 1e-30)


def two_parts(x, axis):
    high = x.astype(jnp.bfloat16)
    low = (x - high.astype(jnp.float32)).astype(jnp.bfloat16)
    return jnp.concatenate([high, low], axis=axis)


def proj_step(f, d0):
    return jnp.dot(jnp.concatenate([f, f], axis=1), d0[...], preferred_element_type=jnp.float32)


def out_step(f, d1):
    return lax.dot_general(
        d1[...],
        jnp.concatenate([f, f], axis=1),
        (((1,), (1,)), ((), ())),
        preferred_element_type=jnp.float32,
    )


def exchange_kernel(
    tp_count,
    entries,
    si_hbm,
    pc_hbm,
    sh_hbm,
    oc_hbm,
    f_hbm,
    wp_hbm,
    wo_hbm,
    mf_hbm,
    ms_hbm,
    first_ref,
    second_ref,
    d0_ref,
    d1_ref,
    gp_ref,
    go_ref,
    pn_ref,
    on_ref,
    fp_ref,
    fo_ref,
    si_ref,
    pc_ref,
    sh_ref,
    oc_ref,
    f_ref,
    wp_ref,
    wo_ref,
    mf_ref,
    ms_ref,
    cp,
    co,
    rows,
    rows_in,
    rows_all,
    part,
    part_code,
    part_in,
    grads,
    sq,
    sq_in,
    top_out,
    top_in,
    top_all,
    in_s,
    bulk_s,
    bulk_r,
    zs_s,
    zs_r,
    zg_s,
    zg_r,
    fs_s,
    fs_r,
    fg_s,
    fg_r,
    n_s,
    n_r,
    ts_s,
    ts_r,
    tg_s,
    tg_r,
):
    fs = lax.axis_index("fs")
    tp = lax.axis_index("tp")
    across_x = fs + 1 - 2 * lax.rem(fs, 2)
    across_y = lax.rem(fs + 2, 4)
    fs_peers = (across_x, across_y, 3 - fs)
    tp_peers = [lax.rem(tp + o, tp_count) for o in range(1, tp_count)]

    def send(src, dst, s_sem, r_sem, where):
        copy = pltpu.make_async_remote_copy(
            src_ref=src, dst_ref=dst, send_sem=s_sem, recv_sem=r_sem, device_id=where, device_id_type=MESH
        )
        copy.start()
        return copy

    barrier = pltpu.get_barrier_semaphore()
    for p in fs_peers:
        pl.semaphore_signal(barrier, inc=1, device_id={"fs": p}, device_id_type=MESH)
    for p in tp_peers:
        pl.semaphore_signal(barrier, inc=1, device_id={"tp": p}, device_id_type=MESH)
    pairs = (
        (wp_hbm, wp_ref),
        (wo_hbm, wo_ref),
        (f_hbm, f_ref),
        (si_hbm, si_ref),
        (oc_hbm, oc_ref),
        (pc_hbm, pc_ref),
        (sh_hbm, sh_ref),
        (mf_hbm, mf_ref),
        (ms_hbm, ms_ref),
    )
    loads = [pltpu.make_async_copy(a, b, in_s.at[i]) for i, (a, b) in enumerate(pairs)]
    for c in loads:
        c.start()
    loads[0].wait()
    cp[...] = encode(wp_ref[...], weight_gain, 4)
    pl.semaphore_wait(barrier, 3 + len(tp_peers))
    bulk = [send(cp, gp_ref.at[0], bulk_s.at[0], bulk_r.at[0], {"fs": across_x})]
    loads[1].wait()
    co[...] = encode(wo_ref[...], weight_gain, 4)
    bulk += [
        send(co, go_ref.at[1], bulk_s.at[1], bulk_r.at[1], {"fs": across_y}),
        send(co, go_ref.at[0], bulk_s.at[2], bulk_r.at[2], {"fs": across_x}),
        send(cp, gp_ref.at[1], bulk_s.at[3], bulk_r.at[3], {"fs": across_y}),
    ]
    for c in loads[2:5]:
        c.wait()

    tokens, feats = si_ref.shape
    own = pl.ds(pl.multiple_of(tp * feats, feats), feats)
    rows[:tokens, :] = jnp.dot(si_ref[...], f_ref[0, own, :], preferred_element_type=jnp.float32)
    rows[tokens:, :] = jnp.dot(oc_ref[...], f_ref[1, own, :], preferred_element_type=jnp.float32)
    piece = rows_in.shape[1]

    def rows_of(i):
        return pl.ds(pl.multiple_of(i * piece, 8), piece)

    copies = [
        send(rows.at[rows_of(p), :], rows_in.at[i], zs_s.at[i], zs_r.at[i], {"tp": p})
        for i, p in enumerate(tp_peers)
    ]
    for c in copies:
        c.wait_recv()
    total = rows[rows_of(tp), :]
    for i in range(tp_count - 1):
        total = total + rows_in[i]
    rows_all[rows_of(tp), :] = total
    gathers = [
        send(rows_all.at[rows_of(tp), :], rows_all.at[rows_of(tp), :], zg_s.at[i], zg_r.at[i], {"tp": p})
        for i, p in enumerate(tp_peers)
    ]
    for c in copies:
        c.wait_send()
    for c in loads[5:]:
        c.wait()
    for c in gathers:
        c.wait_recv()

    rank = f_ref.shape[2]
    slab = part_in.shape[1]
    for k, right in enumerate((pc_ref, sh_ref)):
        left = two_parts(rows_all[k * tokens : (k + 1) * tokens, :], 1)
        both = lax.dot_general(
            left, right[...], (((0,), (0,)), ((), ())), preferred_element_type=jnp.float32
        )
        both = both[:rank] + both[rank:]
        part[k * rank : (k + 1) * rank, :] = both
        for h in range(rank // slab):
            mine = both[h * slab : (h + 1) * slab]
            top = largest(mine)
            start = k * rank + h * slab
            top_out[start // slab] = jnp.broadcast_to(top, sq.shape)
            part_code[start : start + slab, :] = encode(mine, code_top / top, 4)
    for c in gathers:
        c.wait_send()

    def slab_of(i):
        return pl.ds(pl.multiple_of(i * slab, slab), slab)

    copies = [
        send(part_code.at[slab_of(p), :], part_in.at[i], fs_s.at[i], fs_r.at[i], {"fs": p})
        for i, p in enumerate(fs_peers)
    ]
    copies += [
        send(top_out.at[p], top_in.at[i], ts_s.at[i], ts_r.at[i], {"fs": p}) for i, p in enumerate(fs_peers)
    ]
    d_rows, width = cp.shape

    def relay(start, stop, at):
        a = pl.ds(start * d_rows // 8, (stop - start) * d_rows // 8)
        b = pl.ds(start * width // 8, (stop - start) * width // 8)
        return [
            send(gp_ref.at[0, a, :], gp_ref.at[2, a, :], bulk_s.at[at], bulk_r.at[at], {"fs": across_y}),
            send(
                go_ref.at[1, b, :], go_ref.at[2, b, :], bulk_s.at[at + 1], bulk_r.at[at + 1], {"fs": across_x}
            ),
        ]

    bulk[0].wait_recv()
    bulk[1].wait_recv()
    bulk += relay(0, 1, 4)
    for c in copies:
        c.wait_recv()
    total = part[slab_of(fs), :]
    for i in range(3):
        total = total + decode(part_in[i], code_top / top_in[i][0:1, 0:1], 4)
    top = largest(total)
    top_all[fs] = jnp.broadcast_to(top, sq.shape)
    grads[slab_of(fs), :] = encode(total, code_top / top, 4)
    gathers = [
        send(grads.at[slab_of(fs), :], grads.at[slab_of(fs), :], fg_s.at[i], fg_r.at[i], {"fs": p})
        for i, p in enumerate(fs_peers)
    ]
    gathers += [
        send(top_all.at[fs], top_all.at[fs], tg_s.at[i], tg_r.at[i], {"fs": p}) for i, p in enumerate(fs_peers)
    ]
    bulk += relay(1, 8, 6)
    for c in copies:
        c.wait_send()
    for c in gathers:
        c.wait_recv()
    small = jnp.concatenate(
        [
            decode(grads[j * slab : (j + 1) * slab, :], code_top / top_all[j][0:1, 0:1], 4)
            for j in range(2 * rank // slab)
        ],
        axis=0,
    )
    first = beta_first * mf_ref[...] + (1.0 - beta_first) * small
    second = beta_second * ms_ref[...] + (1.0 - beta_second) * small * small
    first_ref[...] = first
    second_ref[...] = second
    direction = first / (jnp.sqrt(second) + epsilon)
    for c in gathers:
        c.wait_send()

    d_model = f_ref.shape[1]
    step = d_model // 8
    squares = []
    for k in range(2):
        thin = two_parts(direction[k * rank : (k + 1) * rank], 0)

        def add(i, acc, k=k, thin=thin):
            f = f_ref[k, pl.ds(pl.multiple_of(i * step, step), step), :]
            u = jnp.dot(jnp.concatenate([f, f], axis=1), thin, preferred_element_type=jnp.float32)
            return acc + jnp.sum(u * u, axis=0, keepdims=True)

        acc = lax.fori_loop(0, 8, add, jnp.zeros((1, width), jnp.float32))
        squares.append(jnp.sum(acc, axis=1, keepdims=True))
    row = lax.broadcasted_iota(jnp.int32, sq.shape, 0)
    sq[...] = jnp.where(row == 0, squares[0], squares[1])
    norms = [send(sq, sq_in.at[i], n_s.at[i], n_r.at[i], {"tp": p}) for i, p in enumerate(tp_peers)]
    for c in norms:
        c.wait_recv()
    total = sq[...]
    for i in range(tp_count - 1):
        total = total + sq_in[i]
    scale = -learn_rate * lax.rsqrt(total / entries + epsilon)
    d0_ref[...] = two_parts(direction[:rank] * scale[0:1, 0:1], 0)
    d1_ref[...] = two_parts(jnp.transpose(direction[rank:] * scale[1:2, 0:1]), 1)
    for c in norms:
        c.wait_send()

    size = d_rows // chunks

    def block(slot, owner, proj_code, out_code):
        def one(i, _):
            at = pl.ds(pl.multiple_of(i * size, size), size)
            there = pl.ds(pl.multiple_of(owner * d_rows + i * size, size), size)
            u = proj_step(f_ref[0, there, :], d0_ref)
            fp_ref[slot, at, :] = (decode(proj_code[at, :], weight_gain, 4) + u).astype(jnp.bfloat16)
            if slot == 0:
                pn_ref[at, :] = wp_ref[at, :] + u
            u = out_step(f_ref[1, there, :], d1_ref)
            fo_ref[slot, :, at] = (decode(out_code[:, at], weight_gain, 4) + u).astype(jnp.bfloat16)
            if slot == 0:
                on_ref[:, at] = wo_ref[:, at] + u
            return 0

        lax.fori_loop(0, chunks, one, 0)

    block(0, fs, cp, co)
    bulk[2].wait_recv()
    block(1, across_x, gp_ref.at[0], go_ref.at[0])
    bulk[3].wait_recv()
    block(2, across_y, gp_ref.at[1], go_ref.at[1])
    for c in bulk[4:]:
        c.wait_recv()
    for c in bulk:
        c.wait_send()


def finish_kernel(
    me_ref, f_ref, d0, d1, gp, go, pn, on, fp, fo, mf, ms,
    pn_hbm, on_hbm, pc_hbm, oc_hbm, first_hbm, second_hbm, last_p, last_o, sems
):
    me = me_ref[0]
    d_rows = pn.shape[0]
    size = d_rows // chunks

    def span(owner, i=0, n=d_rows):
        return pl.ds(pl.multiple_of(owner * d_rows + i * n, n), n)

    owners = (me, me ^ 1, me ^ 2)
    pairs = [(pn, pn_hbm), (on, on_hbm), (mf, first_hbm), (ms, second_hbm)]
    for r, owner in enumerate(owners):
        pairs += [(fp.at[r], pc_hbm.at[span(owner), :]), (fo.at[r], oc_hbm.at[:, span(owner)])]
    copies = [pltpu.make_async_copy(a, b, sems.at[i]) for i, (a, b) in enumerate(pairs)]
    for c in copies:
        c.start()
    for i in range(chunks):
        at = pl.ds(i * size, size)
        there = span(me ^ 3, i, size)
        u = proj_step(f_ref[0, there, :], d0)
        last_p[at, :] = (decode(gp[2, at, :], weight_gain, 4) + u).astype(jnp.bfloat16)
        u = out_step(f_ref[1, there, :], d1)
        last_o[:, at] = (decode(go[2, :, at], weight_gain, 4) + u).astype(jnp.bfloat16)
        for a, b in ((last_p.at[at, :], pc_hbm.at[there, :]), (last_o.at[:, at], oc_hbm.at[:, there])):
            c = pltpu.make_async_copy(a, b, sems.at[len(copies)])
            c.start()
            copies.append(c)
    for c in copies:
        c.wait()


def fast_body(si, pc, sh, oc, factors, w_proj, w_out, m1, m2):
    fs_count, tp_count = lax.axis_size("fs"), lax.axis_size("tp")
    kinds, d_model, rank = factors.shape
    tokens = si.shape[0]
    width = pc.shape[1]
    d_rows = w_proj.shape[0]
    f32, bf16 = jnp.float32, jnp.bfloat16
    mf, ms = m1.reshape(2 * rank, width), m2.reshape(2 * rank, width)
    vm = pl.BlockSpec(memory_space=pltpu.VMEM)
    hbm = pl.BlockSpec(memory_space=pltpu.HBM)
    dma = lambda n: pltpu.SemaphoreType.DMA((n,))
    shape = jax.ShapeDtypeStruct
    peers = tp_count - 1
    piece = 2 * tokens // tp_count
    slab = 2 * rank // fs_count
    args = (si, pc, sh, oc, factors, w_proj, w_out, mf, ms)
    held = tuple(pltpu.with_memory_space_constraint(a, pltpu.HBM) for a in args)
    first, second, d0, d1, gp, go, pn, on, fp, fo = pl.pallas_call(
        functools.partial(exchange_kernel, tp_count, float(d_model * width * tp_count)),
        out_shape=(
            pltpu.VMEM((2 * rank, width), f32),
            pltpu.VMEM((2 * rank, width), f32),
            pltpu.VMEM((2 * rank, width), bf16),
            pltpu.VMEM((width, 2 * rank), bf16),
            pltpu.VMEM((3, d_rows, width), bf16),
            pltpu.VMEM((3, width, d_rows), bf16),
            pltpu.VMEM((d_rows, width), f32),
            pltpu.VMEM((width, d_rows), f32),
            pltpu.VMEM((3, d_rows, width), bf16),
            pltpu.VMEM((3, width, d_rows), bf16),
        ),
        in_specs=[hbm] * 9,
        out_specs=(vm,) * 10,
        scratch_shapes=[pltpu.VMEM(a.shape, a.dtype) for a in args]
        + [
            pltpu.VMEM((d_rows, width), bf16),
            pltpu.VMEM((width, d_rows), bf16),
            pltpu.VMEM((2 * tokens, rank), f32),
            pltpu.VMEM((peers, piece, rank), f32),
            pltpu.VMEM((2 * tokens, rank), f32),
            pltpu.VMEM((2 * rank, width), f32),
            pltpu.VMEM((2 * rank, width), bf16),
            pltpu.VMEM((3, slab, width), bf16),
            pltpu.VMEM((2 * rank, width), bf16),
            pltpu.VMEM((8, 128), f32),
            pltpu.VMEM((peers, 8, 128), f32),
            pltpu.VMEM((fs_count, 8, 128), f32),
            pltpu.VMEM((3, 8, 128), f32),
            pltpu.VMEM((fs_count, 8, 128), f32),
            dma(9),
            dma(8),
            dma(8),
            dma(peers),
            dma(peers),
            dma(peers),
            dma(peers),
            dma(3),
            dma(3),
            dma(3),
            dma(3),
            dma(peers),
            dma(peers),
            dma(3),
            dma(3),
            dma(3),
            dma(3),
        ],
        compiler_params=pltpu.CompilerParams(
            collective_id=0, has_side_effects=True, vmem_limit_bytes=40 * MIB
        ),
        name="exchange",
    )(*held)

    me = lax.axis_index("fs").astype(jnp.int32).reshape(1)
    pn, on, pcopy, ocopy, first, second = pl.pallas_call(
        finish_kernel,
        in_specs=[pl.BlockSpec(memory_space=pltpu.SMEM)] + [vm] * 11,
        out_specs=[hbm] * 6,
        out_shape=(
            shape(w_proj.shape, f32),
            shape(w_out.shape, f32),
            shape((d_model, width), bf16),
            shape((width, d_model), bf16),
            shape((2 * rank, width), f32),
            shape((2 * rank, width), f32),
        ),
        scratch_shapes=[
            pltpu.VMEM((d_rows, width), bf16),
            pltpu.VMEM((width, d_rows), bf16),
            dma(10 + 2 * chunks),
        ],
        compiler_params=pltpu.CompilerParams(vmem_limit_bytes=14 * MIB),
        name="finish",
    )(me, factors, d0, d1, gp, go, pn, on, fp, fo, first, second)
    return pn, on, pcopy, ocopy, first.reshape(m1.shape), second.reshape(m2.shape)


def over_tokens(left_rows, right_rows, precise):
    return lax.dot_general(
        left_rows,
        right_rows,
        (((0,), (0,)), ((), ())),
        preferred_element_type=jnp.float32,
        precision=precise,
    )


def body(
    saved_inputs,
    proj_cotangent,
    saved_hidden,
    out_cotangent,
    factors,
    w_proj,
    w_out,
    moment_first,
    moment_second,
):
    highest = lax.Precision.HIGHEST
    fs_count = lax.axis_size("fs")
    tp_count = lax.axis_size("tp")
    d_model = factors.shape[1]
    hidden_width = proj_cotangent.shape[1]
    fs_rows = d_model // fs_count
    tp_feats = saved_inputs.shape[1]
    own_rows = lax.dynamic_slice_in_dim(factors, lax.axis_index("fs") * fs_rows, fs_rows, 1).astype(
        jnp.float32
    )
    own_feats = lax.dynamic_slice_in_dim(factors, lax.axis_index("tp") * tp_feats, tp_feats, 1)
    proj_rows = jnp.dot(saved_inputs, own_feats[0], preferred_element_type=jnp.float32)
    out_rows = jnp.dot(out_cotangent, own_feats[1], preferred_element_type=jnp.float32)
    proj_rows, out_rows = lax.psum((proj_rows, out_rows), "tp")
    partial_sums = jnp.stack(
        [
            over_tokens(proj_rows, proj_cotangent.astype(jnp.float32), highest),
            over_tokens(out_rows, saved_hidden.astype(jnp.float32), highest),
        ]
    )
    small_grads = lax.psum(partial_sums, "fs")
    first_next = beta_first * moment_first + (1.0 - beta_first) * small_grads
    second_next = beta_second * moment_second + (1.0 - beta_second) * small_grads * small_grads
    direction = first_next / (jnp.sqrt(second_next) + epsilon)
    update_full = jnp.einsum("kdr,kre->kde", own_rows, direction, precision=highest)
    squares = lax.psum(jnp.sum(update_full * update_full, axis=(1, 2)), ("fs", "tp"))
    norm_scale = lax.rsqrt(squares / (d_model * hidden_width * tp_count) + epsilon)
    stepped = update_full * norm_scale[:, None, None]
    proj_next = w_proj - learn_rate * stepped[0]
    out_next = w_out - learn_rate * stepped[1].T
    proj_copy, out_copy = (
        lax.all_gather(proj_next.astype(jnp.bfloat16), "fs", axis=0, tiled=True),
        lax.all_gather(out_next.astype(jnp.bfloat16), "fs", axis=1, tiled=True),
    )
    return (proj_next, out_next, proj_copy, out_copy, first_next, second_next)


def solution(mesh):
    placed = (
        P("fs", "tp"),
        P("fs", "tp"),
        P("fs", "tp"),
        P("fs", "tp"),
        P(),
        P("fs", "tp"),
        P("tp", "fs"),
        P(None, None, "tp"),
        P(None, None, "tp"),
    )
    planned = fast_body if mesh.shape["fs"] == 4 and mesh.shape["tp"] == 8 else body
    return jax.shard_map(
        planned,
        mesh=mesh,
        in_specs=placed,
        out_specs=(
            P("fs", "tp"),
            P("tp", "fs"),
            P(None, "tp"),
            P("tp", None),
            P(None, None, "tp"),
            P(None, None, "tp"),
        ),
        check_vma=False,
    )
```
